32 devices in a mesh: ep: 4 (over y, x), tp: 8 (over z, core).
Axes of the slice: x: 2, y: 2, z: 4, core: 2. Of those that a mesh axis runs over, the one named last changes fastest.
Arguments:
- pool_in: bfloat16 [16384, 1024], P(('ep', 'tp')), may hold values from -6 to 6
- pool_weight: bfloat16 [4, 256, 256], replicated, may hold values from -0.375 to 0.375
- pool_gain: float32 [1024], replicated, may hold values from 0.1 to 1.9
- out_weight: bfloat16 [1024, 2048], P('tp'), may hold values from -0.1875 to 0.1875
- mix_gain: float32 [2048], replicated, may hold values from 0.1 to 1.9
- expert_in: bfloat16 [1024, 2048], P('ep'), may hold values from -6 to 6
- routes: int32 [1024, 4], P('ep'), may hold values from 0 to 7, all different within a row; in each aligned block of 32 rows (0 to 31, 32 to 63, ...) at most 32 rows name the same one
- route_weight: float32 [1024, 4], P('ep'), may hold values from 0.1 to 1
- pre_gain: float32 [2048], replicated, may hold values from 0.1 to 1.9
- gate_weight: bfloat16 [8, 2048, 4096], P('ep', None, 'tp'), may hold values from -0.39648438 to 0.39648438
- up_weight: bfloat16 [8, 2048, 4096], P('ep', None, 'tp'), may hold values from -0.39648438 to 0.39648438
- down_weight: bfloat16 [8, 4096, 2048], P('ep', 'tp'), may hold values from -0.09375 to 0.09375
- post_gain: float32 [2048], replicated, may hold values from 0.1 to 1.9
Outputs:
- mix_out: bfloat16 [16384, 2048], P(('ep', 'tp'))
- expert_out: bfloat16 [1024, 2048], P(('ep', 'tp'))
The draws below stay inside these ranges and needn't reach their ends.
Inputs may be any that keep to these rules, and one draw needn't show every extreme that they name: `routes`: each row names 4 different experts. In each aligned block of 32 rows no expert is named by more than 32 rows, a bound that some block reaches.
All inputs are finite; a program needn't handle non-finite values.
Results may differ from the reference program's by a relative error of at most 0.019.
Values may be sent and summed in bfloat16 or wider, within the bound.
A program may use at most 128 MiB of HBM per device.

```python
import math
import jax
import jax.numpy as jnp
import numpy as np
from jax import lax

D = 2048
DP = 1024
GROUP = 256
FF = 4096
EXPERTS = 8
TOPK = 4
MOE_TOK = 1024
MIX_TOK = 16384
SUB = 32
CAP = 32
N_TP = 8


def shard_levels(rng, dims, cuts, least, high):
    level, own = 1.0, jax.random.fold_in(rng, 6)
    for dim, shards_of in cuts:
        heights = jnp.exp(jax.random.uniform(jax.random.fold_in(own, dim), (shards_of,), jnp.float32, least / len(cuts), high / len(cuts)))
        level = level * jnp.repeat(heights, dims[dim] // shards_of).reshape([-1 if axis == dim else 1 for axis in range(len(dims))])
    return level


def deal_out(rng, own, number, rows, count, top, most, lean):
    order = jax.random.permutation(rng, count)
    heavy_load, common = portions_of(count, rows * top, most, lean, True), portions_of(count, rows * top, most, lean, False)
    places = jnp.arange(count)

    def named(sizes, turn):
        used = int((sizes > 0).sum())
        fixed = max(1, used // 4)
        passed = fixed + (places - fixed + turn * (used - fixed)) % max(1, count - fixed)
        return jnp.zeros((count,), jnp.int32).at[order[jnp.where(places < fixed, places, passed)]].set(jnp.asarray(sizes, jnp.int32))

    sizes = jnp.where(number % 4 == 0, named(heavy_load, number // 4), named(common, number - number // 4 - 1))
    mixed = jax.random.permutation(jax.random.fold_in(own, 3), count)
    giver, sink = mixed[0:count // 2 * 2:2], mixed[1:count // 2 * 2:2]
    margin = jnp.minimum(sizes[giver] - 1, most - sizes[sink]) // 2
    margin = jnp.where((giver == order[0]) | (sink == order[0]) | (sizes[sink] == 0), 0, jnp.maximum(margin, 0))
    passed = jax.random.randint(jax.random.fold_in(own, 4), (count // 2,), 0, 1 << 20) % (margin + 1)
    sizes = sizes.at[giver].add(-passed).at[sink].add(passed)
    labels = jnp.searchsorted(jnp.cumsum(sizes), jnp.arange(rows * top), side="right").astype(jnp.int32)
    listing = labels.reshape(top, rows).T
    listing = listing[jax.random.permutation(jax.random.fold_in(own, 1), rows)]
    turn = jax.random.randint(jax.random.fold_in(own, 2), (rows, 1), 0, top)
    return jnp.take_along_axis(listing, (jnp.arange(top)[None, :] + turn) % top, axis=1)


def portions_of(count, total, limit, lean, full):
    portions = [(1 << 20) // math.isqrt(standing ** lean) + 1 for standing in range(1, count + 1)]
    largest = limit if full else min(limit, max(-(-total // count), total * portions[0] // sum(portions)))
    least = 1 if total - largest >= count - 1 else 0
    given, surplus = [largest] + [least] * (count - 1), total - largest - least * (count - 1)
    while surplus > 0:
        candidates = [i for i in range(1, count) if given[i] < largest] or [i for i in range(1, count) if given[i] < limit]
        pool, left = sum([portions[i] for i in candidates]), surplus
        for i in candidates:
            more = min(limit - given[i], max(1, left * portions[i] // pool), surplus)
            given[i] = given[i] + more
            surplus = surplus - more
    return np.array(given)


def noise(rng, extent, width, most, cuts=(), held_as=jnp.bfloat16):
    level = shard_levels(rng, extent, cuts, -0.22, 0.18) if cuts else 1.0
    array = jax.random.normal(rng, extent, jnp.float32) * width * level
    return jnp.minimum(jnp.maximum(array, -most), most).astype(held_as)


def setup_inputs(seed: int = 0) -> dict:
    splits = jax.random.split(jax.random.key(seed), 14)
    pool_in = noise(splits[0], (MIX_TOK, DP), 1.0, 6.0, ((0, 32),))
    pool_weight = noise(splits[1], (4, GROUP, GROUP), GROUP ** -0.5, 0.375)
    pool_gain = jnp.clip(1.0 + 0.18 * jax.random.normal(splits[2], (DP,), jnp.float32), 0.1, 1.9)
    out_weight = noise(splits[3], (DP, D), DP ** -0.5, 0.1875, ((0, 8),))
    mix_gain = jnp.clip(1.0 + 0.18 * jax.random.normal(splits[4], (D,), jnp.float32), 0.1, 1.9)
    expert_in = noise(splits[5], (MOE_TOK, D), 1.0, 6.0, ((0, 4),))
    routes_keys = jax.random.split(jax.random.fold_in(splits[6], 1), MOE_TOK // SUB)
    routes_turns = jax.random.permutation(jax.random.fold_in(splits[6], 3), MOE_TOK // SUB)
    routes = jax.vmap(lambda own, number: deal_out(jax.random.fold_in(splits[6], 2), own, number, SUB, EXPERTS, TOPK, CAP, 2))(routes_keys, routes_turns).reshape((MOE_TOK, TOPK))
    route_weight = jnp.clip(jnp.exp(math.log(1.0) - 2.3025851 * jax.random.uniform(splits[7], (MOE_TOK, TOPK), jnp.float32) ** shard_levels(splits[7], (MOE_TOK, TOPK), ((0, 4),), -0.2, 0.2)), 0.1, 1.0)
    pre_gain = jnp.clip(1.0 + 0.18 * jax.random.normal(splits[8], (D,), jnp.float32), 0.1, 1.9)
    gate_weight = noise(splits[9], (EXPERTS, D, FF), (3.0 * D ** -0.5), 0.39648438, ((0, 4), (2, 8)))
    up_weight = noise(splits[10], (EXPERTS, D, FF), (3.0 * D ** -0.5), 0.39648438, ((0, 4), (2, 8)))
    down_weight = noise(splits[11], (EXPERTS, FF, D), FF ** -0.5, 0.09375, ((0, 4), (1, 8)))
    post_gain = jnp.clip(1.0 + 0.18 * jax.random.normal(splits[12], (D,), jnp.float32), 0.1, 1.9)
    return {"pool_in": pool_in, "pool_weight": pool_weight, "pool_gain": pool_gain, "out_weight": out_weight, "mix_gain": mix_gain, "expert_in": expert_in, "routes": routes, "route_weight": route_weight, "pre_gain": pre_gain, "gate_weight": gate_weight, "up_weight": up_weight, "down_weight": down_weight, "post_gain": post_gain}


WINDOWS = (2, 4, 8, 16)
EPS = 1e-06
LIMIT = 7.0
ALPHA = 1.702

def rms_scale(values, gain):
    mean_square = lax.optimization_barrier(jnp.mean(values * values, axis=-1, keepdims=True))
    return values * lax.rsqrt(mean_square + EPS) * gain.astype(jnp.float32)

def trailing_pool(padded, first_pos, rows):
    group = padded.shape[1] // 4
    position = first_pos + jnp.arange(rows, dtype=jnp.int32)
    pieces = []
    for which, window in enumerate(WINDOWS):
        channels = padded[:, which * group:(which + 1) * group]
        running = channels[16:16 + rows]
        for reach in range(2, window + 1):
            running = running + channels[17 - reach:17 - reach + rows]
        count = jnp.minimum(position + 1, window).astype(jnp.float32)[:, None]
        pieces.append(running / count)
    pooled = jnp.concatenate(pieces, axis=1)
    return (pooled - padded[16:]).astype(jnp.bfloat16)

def selection(block_routes, experts, capacity):
    flat = block_routes.reshape(-1)
    onehot = (flat[:, None] == jnp.arange(experts, dtype=jnp.int32)[None, :]).astype(jnp.int32)
    earlier = jnp.cumsum(onehot, axis=0) - onehot
    rank = lax.optimization_barrier(jnp.sum(earlier * onehot, axis=1))
    slots = (flat * capacity + rank).reshape(block_routes.shape)
    return (slots[:, :, None] == jnp.arange(experts * capacity, dtype=jnp.int32)[None, None, :]).astype(jnp.bfloat16)

def clamped_unit(gate, up):
    gate = jnp.minimum(gate, LIMIT)
    up = jnp.clip(up, -LIMIT, LIMIT)
    return (up + 1.0) * gate * jax.nn.sigmoid(ALPHA * gate)

def expert_rows(rows, gate_w, up_w, down_w):
    gate = jnp.dot(rows, gate_w, preferred_element_type=jnp.float32)
    up = jnp.dot(rows, up_w, preferred_element_type=jnp.float32)
    hidden = clamped_unit(gate, up).astype(jnp.bfloat16)
    parts = hidden.reshape(rows.shape[0], N_TP, FF // N_TP).astype(jnp.float32)
    slices = down_w.reshape(N_TP, FF // N_TP, D).astype(jnp.float32)
    partial_value = jnp.einsum('rtf,tfd->rtd', parts, slices).astype(jnp.bfloat16)
    partial_value = lax.optimization_barrier(partial_value)
    return lax.optimization_barrier(jnp.sum(partial_value.astype(jnp.float32), axis=1)).astype(jnp.bfloat16)

def reference(pool_in, pool_weight, pool_gain, out_weight, mix_gain, expert_in, routes, route_weight, pre_gain, gate_weight, up_weight, down_weight, post_gain):
    rows = pool_in.shape[0]
    padded = jnp.concatenate([jnp.zeros((16, pool_in.shape[1]), jnp.float32), pool_in.astype(jnp.float32)], axis=0)
    diff = trailing_pool(padded, jnp.int32(0), rows)
    grouped = diff.reshape(rows, 4, GROUP).astype(jnp.float32)
    mixed = jnp.einsum('sgc,gcd->sgd', grouped, pool_weight.astype(jnp.float32))
    mixed = (mixed.reshape(rows, DP) * pool_gain.astype(jnp.float32)).astype(jnp.bfloat16)
    projected = jnp.dot(mixed, out_weight, preferred_element_type=jnp.float32)
    mix_out = rms_scale(projected, mix_gain).astype(jnp.bfloat16)
    normed = rms_scale(expert_in.astype(jnp.float32), pre_gain).astype(jnp.bfloat16)
    blocks = routes.shape[0] // SUB
    picks = jax.vmap(lambda block: selection(block, EXPERTS, CAP))(routes.reshape(blocks, SUB, TOPK)).astype(jnp.float32)
    token_picks = lax.optimization_barrier(jnp.sum(picks, axis=2))
    buffers = jnp.einsum('bts,btd->bsd', token_picks, normed.reshape(blocks, SUB, D).astype(jnp.float32)).astype(jnp.bfloat16)
    gathered = buffers.reshape(blocks, EXPERTS, CAP, D).transpose(1, 0, 2, 3).reshape(EXPERTS, blocks * CAP, D)
    outputs = lax.map(lambda operands: expert_rows(*operands), (gathered, gate_weight, up_weight, down_weight))
    back = outputs.reshape(EXPERTS, blocks, CAP, D).transpose(1, 0, 2, 3).reshape(blocks, EXPERTS * CAP, D).astype(jnp.float32)
    per_route = jnp.einsum('btks,bsd->btkd', picks, back)
    weights = route_weight.reshape(blocks, SUB, TOPK).astype(jnp.float32)
    combined = lax.optimization_barrier(jnp.sum(per_route * weights[..., None], axis=2)).reshape(blocks * SUB, D)
    expert_out = rms_scale(combined, post_gain).astype(jnp.bfloat16)
    return (mix_out, expert_out)
```

```python
import jax
import jax.numpy as jnp
from jax import lax
from jax.sharding import PartitionSpec as P

WINDOWS = (2, 4, 8, 16)
EPS = 1e-06
LIMIT = 7.0
ALPHA = 1.702


def shifted(block, axis, distance):
    devices = range(lax.axis_size(axis))
    route = [(i - distance, i) for i in devices if i - distance in devices]
    return lax.ppermute(block, axis, route)


def rms_scale(values, gain):
    mean_square = jnp.mean(values * values, axis=-1, keepdims=True)
    return values * lax.rsqrt(mean_square + EPS) * gain


def trailing_pool(padded, first_pos, rows):
    group = padded.shape[1] // 4
    position = first_pos + jnp.arange(rows, dtype=jnp.int32)
    pieces = []
    for which, window in enumerate(WINDOWS):
        channels = padded[:, which * group : (which + 1) * group]
        running = channels[16 : 16 + rows]
        for reach in range(2, window + 1):
            running = running + channels[17 - reach : 17 - reach + rows]
        count = jnp.minimum(position + 1, window).astype(jnp.float32)[:, None]
        pieces.append(running / count)
    pooled = jnp.concatenate(pieces, axis=1)
    return (pooled - padded[16:]).astype(jnp.bfloat16)


def expert_weights(routes, route_weight, experts):
    chosen = routes[:, :, None] == jnp.arange(experts, dtype=jnp.int32)[None, None, :]
    return jnp.sum(jnp.where(chosen, route_weight[:, :, None], 0.0), axis=1)


def clamped_unit(gate, up):
    gate = jnp.minimum(gate, LIMIT)
    up = jnp.clip(up, -LIMIT, LIMIT)
    return (up + 1.0) * gate * jax.nn.sigmoid(ALPHA * gate)


def body(
    pool_in,
    pool_weight,
    pool_gain,
    out_weight,
    mix_gain,
    expert_in,
    routes,
    route_weight,
    pre_gain,
    gate_weight,
    up_weight,
    down_weight,
    post_gain,
):
    rows, channels = pool_in.shape
    width = out_weight.shape[1]
    rim = shifted(pool_in[rows - 16 :], ("ep", "tp"), 1)
    padded = jnp.concatenate([rim, pool_in], axis=0).astype(jnp.float32)
    first_pos = (lax.axis_index("ep") * lax.axis_size("tp") + lax.axis_index("tp")) * rows
    diff = trailing_pool(padded, first_pos, rows)
    mixed = jnp.einsum(
        "sgc,gcd->sgd",
        diff.reshape(rows, 4, channels // 4),
        pool_weight,
        preferred_element_type=jnp.float32,
    )
    mixed = (mixed.reshape(rows, channels) * pool_gain).astype(jnp.bfloat16)
    projected = jnp.dot(
        mixed,
        lax.all_gather(out_weight, "tp", axis=0, tiled=True),
        preferred_element_type=jnp.float32,
    )
    mix_out = rms_scale(projected, mix_gain).astype(jnp.bfloat16)
    ep_place = lax.axis_index("ep")
    local_experts = gate_weight.shape[0]
    experts = local_experts * lax.axis_size("ep")
    weights = expert_weights(routes, route_weight, experts)
    weights = lax.all_gather(weights, "ep", axis=0, tiled=True)
    weights = lax.dynamic_slice_in_dim(weights, ep_place * local_experts, local_experts, 1)
    normed = rms_scale(expert_in.astype(jnp.float32), pre_gain).astype(jnp.bfloat16)
    normed = lax.all_gather(normed, "ep", axis=0, tiled=True)
    hidden = []
    for which in range(local_experts):
        gate = jnp.dot(normed, gate_weight[which], preferred_element_type=jnp.float32)
        up = jnp.dot(normed, up_weight[which], preferred_element_type=jnp.float32)
        hidden.append(
            (clamped_unit(gate, up) * weights[:, which : which + 1]).astype(jnp.bfloat16)
        )
    hidden = jnp.concatenate(hidden, axis=1)
    partial = jnp.dot(
        hidden, down_weight.reshape(-1, width), preferred_element_type=jnp.float32
    ).astype(jnp.bfloat16)
    combined = lax.psum_scatter(
        partial, ("ep", "tp"), scatter_dimension=0, tiled=True
    ).astype(jnp.float32)
    expert_out = rms_scale(combined, post_gain).astype(jnp.bfloat16)
    return (mix_out, expert_out)


def solution(mesh):
    return jax.shard_map(
        body,
        mesh=mesh,
        in_specs=(
            P(("ep", "tp"), None),
            P(),
            P(),
            P("tp", None),
            P(),
            P("ep", None),
            P("ep", None),
            P("ep", None),
            P(),
            P("ep", None, "tp"),
            P("ep", None, "tp"),
            P("ep", "tp", None),
            P(),
        ),
        out_specs=(P(("ep", "tp"), None), P(("ep", "tp"), None)),
        check_vma=False,
    )
```

```python
import functools

import jax
import jax.numpy as jnp
from jax import lax
from jax.experimental import pallas as pl
from jax.experimental.pallas import tpu as pltpu
from jax.sharding import PartitionSpec as P

WINDOWS = (2, 4, 8, 16)
EPS = 1e-06
LIMIT = 7.0
ALPHA = 1.702
LANES = 128
TILE = 512
MESH = pl.DeviceIdType.MESH


def shifted(block, axis, distance):
    devices = range(lax.axis_size(axis))
    route = [(i - distance, i) for i in devices if i - distance in devices]
    return lax.ppermute(block, axis, route)


def rms_scale(values, gain):
    mean_square = jnp.mean(values * values, axis=-1, keepdims=True)
    return values * lax.rsqrt(mean_square + EPS) * gain


def trailing_pool(padded, first_pos, rows):
    group = padded.shape[1] // 4
    position = first_pos + jnp.arange(rows, dtype=jnp.int32)
    pieces = []
    for which, window in enumerate(WINDOWS):
        channels = padded[:, which * group : (which + 1) * group]
        running = channels[16 : 16 + rows]
        for reach in range(2, window + 1):
            running = running + channels[17 - reach : 17 - reach + rows]
        count = jnp.minimum(position + 1, window).astype(jnp.float32)[:, None]
        pieces.append(running / count)
    pooled = jnp.concatenate(pieces, axis=1)
    return (pooled - padded[16:]).astype(jnp.bfloat16)


def expert_weights(routes, route_weight, experts):
    chosen = routes[:, :, None] == jnp.arange(experts, dtype=jnp.int32)[None, None, :]
    return jnp.sum(jnp.where(chosen, route_weight[:, :, None], 0.0), axis=1)


def clamped_unit(gate, up):
    gate = jnp.minimum(gate, LIMIT)
    up = jnp.clip(up, -LIMIT, LIMIT)
    return (up + 1.0) * gate * jax.nn.sigmoid(ALPHA * gate)


def flipped(place, mask, count):
    result, bit = 0, 1
    while bit < count:
        result = result + ((place // bit + mask // bit) % 2) * bit
        bit *= 2
    return result


def expert_kernel(
    n_ep,
    n_tp,
    own_ref,
    gate_hbm,
    up_hbm,
    down_hbm,
    gain_ref,
    out_ref,
    x_ref,
    gate_ref,
    up_ref,
    down_ref,
    hid_ref,
    part_ref,
    core_ref,
    peer_ref,
    acc_ref,
    zsend_ref,
    zrecv_ref,
    load_sem,
    ag_send,
    ag_recv,
    fw_send,
    fw_recv,
    cs_send,
    cs_recv,
    ep_send,
    ep_recv,
    z_send,
    z_recv,
):
    ep, tp = lax.axis_index("ep"), lax.axis_index("tp")
    core, z = tp % 2, tp // 2
    partner = z * 2 + 1 - core
    n_z = n_tp // 2
    tokens = own_ref.shape[0]
    experts, width, units = gate_ref.shape
    tiles = width // TILE
    half = pl.ds(pl.multiple_of(core * (tokens // 2), tokens // 2), tokens // 2)
    last = n_ep - 1

    loads = [
        pltpu.make_async_copy(gate_hbm, gate_ref, load_sem.at[0]),
        pltpu.make_async_copy(up_hbm, up_ref, load_sem.at[1]),
        pltpu.make_async_copy(down_hbm, down_ref, load_sem.at[2]),
    ]
    for load in loads:
        load.start()

    def ep_peer(k):
        return {"ep": flipped(ep, k + 1, n_ep)}

    def z_peer(k):
        return flipped(z, k + 1, n_z)

    barrier = pltpu.get_barrier_semaphore()
    pl.semaphore_signal(barrier, inc=1, device_id={"tp": partner}, device_id_type=MESH)
    for k in range(n_ep - 1):
        pl.semaphore_signal(barrier, inc=1, device_id=ep_peer(k), device_id_type=MESH)
    for k in range(n_z - 1):
        pl.semaphore_signal(
            barrier, inc=1, device_id={"tp": z_peer(k) * 2 + core}, device_id_type=MESH
        )
    pl.semaphore_wait(barrier, n_ep + n_z - 1)

    def gather_copy(k):
        return pltpu.make_async_remote_copy(
            own_ref.at[half],
            x_ref.at[k, half],
            ag_send.at[k],
            ag_recv.at[k],
            device_id=ep_peer(k),
            device_id_type=MESH,
        )

    def forward_copy(k):
        return pltpu.make_async_remote_copy(
            x_ref.at[k, half],
            x_ref.at[k, half],
            fw_send.at[k],
            fw_recv.at[k],
            device_id={"tp": partner},
            device_id_type=MESH,
        )

    def core_copy(k, j):
        return pltpu.make_async_remote_copy(
            part_ref.at[j, :, 1 - core],
            core_ref.at[k, j],
            cs_send.at[j],
            cs_recv.at[k, j],
            device_id={"tp": partner},
            device_id_type=MESH,
        )

    def peer_copy(k):
        return pltpu.make_async_remote_copy(
            core_ref.at[k],
            peer_ref.at[k],
            ep_send.at[k],
            ep_recv.at[k],
            device_id=ep_peer(k),
            device_id_type=MESH,
        )

    def z_copy(k):
        return pltpu.make_async_remote_copy(
            zsend_ref.at[z_peer(k)],
            zrecv_ref.at[k],
            z_send.at[k],
            z_recv.at[k],
            device_id={"tp": z_peer(k) * 2 + core},
            device_id_type=MESH,
        )

    for k in range(n_ep - 1):
        gather_copy(k).start()

    def compute(k, rows):
        lane = lax.broadcasted_iota(jnp.int32, (tokens, LANES), 1) % (LANES // 2)
        packed = rows[:, width:].astype(jnp.float32)

        @pl.loop(0, experts)
        def _(which):
            weight = jnp.sum(
                jnp.where(lane == ep * experts + which, packed, 0.0), axis=1, keepdims=True
            )
            values = rows[:, :width]
            gate = jnp.dot(values, gate_ref[which], preferred_element_type=jnp.float32)
            up = jnp.dot(values, up_ref[which], preferred_element_type=jnp.float32)
            hid_ref[which] = (clamped_unit(gate, up) * weight).astype(jnp.bfloat16)

        @pl.loop(0, tiles)
        def _(j):
            columns = pl.ds(pl.multiple_of(j * TILE, TILE), TILE)
            total = jnp.dot(
                hid_ref[0], down_ref[0, :, columns], preferred_element_type=jnp.float32
            )
            for which in range(1, experts):
                total = total + jnp.dot(
                    hid_ref[which], down_ref[which, :, columns], preferred_element_type=jnp.float32
                )
            part_ref[j] = total.astype(jnp.bfloat16).reshape(part_ref.shape[1:])
            core_copy(k, j).start()

    for load in loads:
        load.wait()
    compute(last, own_ref)

    @pl.loop(0, tiles)
    def _(j):
        core_copy(last, j).wait()
        acc_ref[j] = part_ref[j, :, core].astype(jnp.float32) + core_ref[last, j].astype(
            jnp.float32
        )

    @pl.loop(0, n_ep - 1)
    def _(k):
        gather_copy(k).wait_recv()
        forward_copy(k).start()
        forward_copy(k).wait_recv()
        compute(k, x_ref.at[k])

        @pl.loop(0, tiles)
        def _(j):
            core_copy(k, j).wait()
            core_ref[k, j] = (
                part_ref[j, :, core].astype(jnp.float32) + core_ref[k, j].astype(jnp.float32)
            ).astype(jnp.bfloat16)

        peer_copy(k).start()

    @pl.loop(0, n_ep - 1)
    def _(k):
        peer_copy(k).wait_recv()
        acc_ref[...] += peer_ref[k].astype(jnp.float32)

    for place in range(n_z):
        zsend_ref[place] = acc_ref[:, place].astype(jnp.bfloat16)
    for k in range(n_z - 1):
        z_copy(k).start()
    total = acc_ref[:, z]
    for k in range(n_z - 1):
        z_copy(k).wait_recv()
        total = total + zrecv_ref[k].astype(jnp.float32)
    squares = jnp.sum(jnp.sum(total * total, axis=0), axis=-1, keepdims=True)
    scale = lax.rsqrt(squares / width + EPS)
    for j in range(tiles):
        columns = slice(j * TILE, (j + 1) * TILE)
        out_ref[:, columns] = (total[j] * scale * gain_ref[:, columns]).astype(jnp.bfloat16)

    @pl.loop(0, n_ep - 1)
    def _(k):
        gather_copy(k).wait_send()
        forward_copy(k).wait_send()
        peer_copy(k).wait_send()

    for k in range(n_z - 1):
        z_copy(k).wait_send()


def experts_mixed(own, gate_weight, up_weight, down_weight, gain, n_ep, n_tp):
    tokens, wide = own.shape
    experts, width, units = gate_weight.shape
    tiles, n_z, block = width // TILE, n_tp // 2, tokens // n_tp
    dma = pltpu.SemaphoreType.DMA
    vmem = pl.BlockSpec(memory_space=pltpu.VMEM)
    hbm = pl.BlockSpec(memory_space=pl.ANY)
    bf16 = jnp.bfloat16
    return pl.pallas_call(
        functools.partial(expert_kernel, n_ep, n_tp),
        out_shape=jax.ShapeDtypeStruct((block, width), bf16),
        in_specs=[vmem, hbm, hbm, hbm, vmem],
        out_specs=vmem,
        scratch_shapes=[
            pltpu.VMEM((n_ep - 1, tokens, wide), bf16),
            pltpu.VMEM(gate_weight.shape, bf16),
            pltpu.VMEM(up_weight.shape, bf16),
            pltpu.VMEM(down_weight.shape, bf16),
            pltpu.VMEM((experts, tokens, units), bf16),
            pltpu.VMEM((tiles, n_z, 2, block, TILE), bf16),
            pltpu.VMEM((n_ep, tiles, n_z, block, TILE), bf16),
            pltpu.VMEM((n_ep - 1, tiles, n_z, block, TILE), bf16),
            pltpu.VMEM((tiles, n_z, block, TILE), jnp.float32),
            pltpu.VMEM((n_z, tiles, block, TILE), bf16),
            pltpu.VMEM((n_z - 1, tiles, block, TILE), bf16),
            dma((3,)),
            dma((n_ep - 1,)),
            dma((n_ep - 1,)),
            dma((n_ep - 1,)),
            dma((n_ep - 1,)),
            dma((tiles,)),
            dma((n_ep, tiles)),
            dma((n_ep - 1,)),
            dma((n_ep - 1,)),
            dma((n_z - 1,)),
            dma((n_z - 1,)),
        ],
        compiler_params=pltpu.CompilerParams(
            collective_id=0, has_side_effects=True, vmem_limit_bytes=60 * 2**20
        ),
        cost_estimate=pl.CostEstimate(
            flops=6 * n_ep * tokens * experts * units * width,
            bytes_accessed=64 * 2**20,
            transcendentals=0,
        ),
        name="experts",
    )(own, gate_weight, up_weight, down_weight, gain)


def body(
    pool_in,
    pool_weight,
    pool_gain,
    out_weight,
    mix_gain,
    expert_in,
    routes,
    route_weight,
    pre_gain,
    gate_weight,
    up_weight,
    down_weight,
    post_gain,
):
    rows, channels = pool_in.shape
    width = out_weight.shape[1]
    rim = shifted(pool_in[rows - 16 :], ("ep", "tp"), 1)
    padded = jnp.concatenate([rim, pool_in], axis=0).astype(jnp.float32)
    first_pos = (lax.axis_index("ep") * lax.axis_size("tp") + lax.axis_index("tp")) * rows
    diff = trailing_pool(padded, first_pos, rows)
    mixed = jnp.einsum(
        "sgc,gcd->sgd",
        diff.reshape(rows, 4, channels // 4),
        pool_weight,
        preferred_element_type=jnp.float32,
    )
    mixed = (mixed.reshape(rows, channels) * pool_gain).astype(jnp.bfloat16)
    projected = jnp.dot(
        mixed,
        lax.all_gather(out_weight, "tp", axis=0, tiled=True),
        preferred_element_type=jnp.float32,
    )
    mix_out = rms_scale(projected, mix_gain).astype(jnp.bfloat16)
    n_ep, n_tp = lax.axis_size("ep"), lax.axis_size("tp")
    experts = gate_weight.shape[0] * n_ep
    weights = expert_weights(routes, route_weight, experts)
    high = lax.reduce_precision(weights, 8, 7)
    fill = ((0, 0), (0, LANES // 2 - experts))
    normed = rms_scale(expert_in.astype(jnp.float32), pre_gain)
    own = jnp.concatenate(
        [normed, jnp.pad(high, fill), jnp.pad(weights - high, fill)], axis=1
    ).astype(jnp.bfloat16)
    expert_out = experts_mixed(
        own, gate_weight, up_weight, down_weight, post_gain[None, :], n_ep, n_tp
    )
    return (mix_out, expert_out)


def solution(mesh):
    return jax.shard_map(
        body,
        mesh=mesh,
        in_specs=(
            P(("ep", "tp"), None),
            P(),
            P(),
            P("tp", None),
            P(),
            P("ep", None),
            P("ep", None),
            P("ep", None),
            P(),
            P("ep", None, "tp"),
            P("ep", None, "tp"),
            P("ep", "tp", None),
            P(),
        ),
        out_specs=(P(("ep", "tp"), None), P(("ep", "tp"), None)),
        check_vma=False,
    )
```

```python
import functools

import jax
import jax.numpy as jnp
from jax import lax
from jax.experimental import pallas as pl
from jax.experimental.pallas import tpu as pltpu
from jax.sharding import PartitionSpec as P

WINDOWS = (2, 4, 8, 16)
EPS = 1e-06
LIMIT = 7.0
ALPHA = 1.702
LANES = 128
TILE = 512
POOL_ROWS = 128
PROJECT_ROWS = 256
MESH = pl.DeviceIdType.MESH


def rms_scale(values, gain):
    mean_square = jnp.mean(values * values, axis=-1, keepdims=True)
    return values * lax.rsqrt(mean_square + EPS) * gain


def expert_weights(routes, route_weight, experts):
    chosen = routes[:, :, None] == jnp.arange(experts, dtype=jnp.int32)[None, None, :]
    return jnp.sum(jnp.where(chosen, route_weight[:, :, None], 0.0), axis=1)


def clamped_unit(gate, up):
    gate = jnp.minimum(gate, LIMIT)
    up = jnp.clip(up, -LIMIT, LIMIT)
    return (up + 1.0) * gate * jax.nn.sigmoid(ALPHA * gate)


def flipped(place, mask, count):
    result, bit = 0, 1
    while bit < count:
        result = result + ((place // bit + mask // bit) % 2) * bit
        bit *= 2
    return result


def expert_kernel(
    n_ep,
    n_tp,
    expert_in_ref,
    packed_ref,
    pre_gain_ref,
    gate_hbm,
    up_hbm,
    down_hbm,
    gain_ref,
    pool_ref,
    pool_weight_ref,
    pool_gain_ref,
    out_weight_ref,
    mix_gain_ref,
    mix_ref,
    out_ref,
    own_ref,
    rim_ref,
    padded_ref,
    mixed_ref,
    all_weight_ref,
    x_ref,
    gate_ref,
    up_ref,
    down_ref,
    hid_ref,
    part_ref,
    core_ref,
    peer_ref,
    acc_ref,
    zsend_ref,
    zrecv_ref,
    load_sem,
    ag_send,
    ag_recv,
    fw_send,
    fw_recv,
    cs_send,
    cs_recv,
    ep_send,
    ep_recv,
    z_send,
    z_recv,
    rim_send,
    rim_recv,
    w_send,
    w_recv,
    wf_send,
    wf_recv,
):
    ep, tp = lax.axis_index("ep"), lax.axis_index("tp")
    core, z = tp % 2, tp // 2
    partner = z * 2 + 1 - core
    n_z = n_tp // 2
    tokens = own_ref.shape[0]
    experts, width, units = gate_ref.shape
    tiles = width // TILE
    half = pl.ds(pl.multiple_of(core * (tokens // 2), tokens // 2), tokens // 2)
    last = n_ep - 1

    loads = [
        pltpu.make_async_copy(gate_hbm, gate_ref, load_sem.at[0]),
        pltpu.make_async_copy(up_hbm, up_ref, load_sem.at[1]),
        pltpu.make_async_copy(down_hbm, down_ref, load_sem.at[2]),
    ]
    for load in loads:
        load.start()

    def ep_peer(k):
        return {"ep": flipped(ep, k + 1, n_ep)}

    def z_peer(k):
        return flipped(z, k + 1, n_z)

    place = ep * n_tp + tp
    devices = n_ep * n_tp
    after, before = (place + 1) % devices, (place + devices - 1) % devices

    def at(device):
        return {"ep": device // n_tp, "tp": device % n_tp}

    barrier = pltpu.get_barrier_semaphore()
    pl.semaphore_signal(barrier, inc=1, device_id=at(after), device_id_type=MESH)
    pl.semaphore_signal(barrier, inc=1, device_id=at(before), device_id_type=MESH)
    pl.semaphore_signal(barrier, inc=1, device_id={"tp": partner}, device_id_type=MESH)
    for k in range(n_ep - 1):
        pl.semaphore_signal(barrier, inc=1, device_id=ep_peer(k), device_id_type=MESH)
    for k in range(n_z - 1):
        pl.semaphore_signal(
            barrier, inc=1, device_id={"tp": z_peer(k) * 2 + core}, device_id_type=MESH
        )
    own_ref[:, :width] = rms_scale(
        expert_in_ref[...].astype(jnp.float32), pre_gain_ref[...]
    ).astype(jnp.bfloat16)
    own_ref[:, width:] = packed_ref[...]
    pl.semaphore_wait(barrier, n_ep + n_z + 1)

    def gather_copy(k):
        return pltpu.make_async_remote_copy(
            own_ref.at[half],
            x_ref.at[k, half],
            ag_send.at[k],
            ag_recv.at[k],
            device_id=ep_peer(k),
            device_id_type=MESH,
        )

    def forward_copy(k):
        return pltpu.make_async_remote_copy(
            x_ref.at[k, half],
            x_ref.at[k, half],
            fw_send.at[k],
            fw_recv.at[k],
            device_id={"tp": partner},
            device_id_type=MESH,
        )

    def core_copy(k, j):
        return pltpu.make_async_remote_copy(
            part_ref.at[j, :, 1 - core],
            core_ref.at[k, j],
            cs_send.at[j],
            cs_recv.at[k, j],
            device_id={"tp": partner},
            device_id_type=MESH,
        )

    def peer_copy(k):
        return pltpu.make_async_remote_copy(
            core_ref.at[k],
            peer_ref.at[k],
            ep_send.at[k],
            ep_recv.at[k],
            device_id=ep_peer(k),
            device_id_type=MESH,
        )

    def z_copy(k):
        return pltpu.make_async_remote_copy(
            zsend_ref.at[z_peer(k)],
            zrecv_ref.at[k],
            z_send.at[k],
            z_recv.at[k],
            device_id={"tp": z_peer(k) * 2 + core},
            device_id_type=MESH,
        )

    rows, channels = pool_ref.shape
    rim_copy = pltpu.make_async_remote_copy(
        pool_ref.at[pl.ds(rows - 16, 16)],
        rim_ref,
        rim_send,
        rim_recv,
        device_id=at(after),
        device_id_type=MESH,
    )

    def weight_copy(k):
        return pltpu.make_async_remote_copy(
            out_weight_ref,
            all_weight_ref.at[tp],
            w_send.at[k],
            w_recv.at[k],
            device_id={"tp": z_peer(k) * 2 + core},
            device_id_type=MESH,
        )

    def weight_forward(k):
        if k == n_z - 1:
            source, target = out_weight_ref, all_weight_ref.at[tp]
        else:
            target = all_weight_ref.at[z_peer(k) * 2 + core]
            source = target
        return pltpu.make_async_remote_copy(
            source,
            target,
            wf_send.at[k],
            wf_recv.at[k],
            device_id={"tp": partner},
            device_id_type=MESH,
        )

    for k in range(n_ep - 1):
        gather_copy(k).start()
    rim_copy.start()
    for k in range(n_z - 1):
        weight_copy(k).start()
    weight_forward(n_z - 1).start()

    def pool():
        padded_ref[: POOL_ROWS - 16] = jnp.zeros((POOL_ROWS - 16, channels), jnp.bfloat16)
        rim_copy.wait_recv()

        @pl.when(place == 0)
        def _():
            padded_ref[POOL_ROWS - 16 : POOL_ROWS] = jnp.zeros((16, channels), jnp.bfloat16)

        @pl.when(place != 0)
        def _():
            padded_ref[POOL_ROWS - 16 : POOL_ROWS] = rim_ref[...]

        padded_ref[POOL_ROWS:] = pool_ref[...]
        group = channels // 4
        reach = (
            lax.broadcasted_iota(jnp.int32, (POOL_ROWS, 2 * POOL_ROWS), 0)
            + POOL_ROWS
            - lax.broadcasted_iota(jnp.int32, (POOL_ROWS, 2 * POOL_ROWS), 1)
        )
        local = lax.broadcasted_iota(jnp.int32, (POOL_ROWS, 1), 0)

        @pl.loop(0, rows // POOL_ROWS)
        def _(i):
            start = pl.multiple_of(i * POOL_ROWS, POOL_ROWS)
            here = pl.ds(start, POOL_ROWS)
            position = place * rows + start + local
            for which, window in enumerate(WINDOWS):
                columns = slice(which * group, (which + 1) * group)
                band = jnp.where((reach >= 0) & (reach < window), 1.0, 0.0).astype(jnp.bfloat16)
                running = jnp.dot(
                    band,
                    padded_ref[pl.ds(start, 2 * POOL_ROWS), columns],
                    preferred_element_type=jnp.float32,
                )
                count = jnp.minimum(position + 1, window).astype(jnp.float32)
                diff = running / count - pool_ref[here, columns].astype(jnp.float32)
                mixed = jnp.dot(
                    diff.astype(jnp.bfloat16),
                    pool_weight_ref[which],
                    preferred_element_type=jnp.float32,
                )
                mixed_ref[here, columns] = (mixed * pool_gain_ref[:, columns]).astype(jnp.bfloat16)

    def project():
        all_weight_ref[tp] = out_weight_ref[...]
        for k in range(n_z - 1):
            weight_copy(k).wait_recv()
            weight_forward(k).start()
        for k in range(n_z):
            weight_forward(k).wait_recv()

        @pl.loop(0, rows // PROJECT_ROWS)
        def _(i):
            here = pl.ds(pl.multiple_of(i * PROJECT_ROWS, PROJECT_ROWS), PROJECT_ROWS)
            projected = jnp.dot(
                mixed_ref[here],
                all_weight_ref[...].reshape(channels, width),
                preferred_element_type=jnp.float32,
            )
            mix_ref[here] = rms_scale(projected, mix_gain_ref[...]).astype(jnp.bfloat16)

    def compute(k, rows):
        lane = lax.broadcasted_iota(jnp.int32, (tokens, LANES), 1) % (LANES // 2)
        packed = rows[:, width:].astype(jnp.float32)

        @pl.loop(0, experts)
        def _(which):
            weight = jnp.sum(
                jnp.where(lane == ep * experts + which, packed, 0.0), axis=1, keepdims=True
            )
            values = rows[:, :width]
            gate = jnp.dot(values, gate_ref[which], preferred_element_type=jnp.float32)
            up = jnp.dot(values, up_ref[which], preferred_element_type=jnp.float32)
            hid_ref[which] = (clamped_unit(gate, up) * weight).astype(jnp.bfloat16)

        @pl.loop(0, tiles)
        def _(j):
            columns = pl.ds(pl.multiple_of(j * TILE, TILE), TILE)
            total = jnp.dot(
                hid_ref[0], down_ref[0, :, columns], preferred_element_type=jnp.float32
            )
            for which in range(1, experts):
                total = total + jnp.dot(
                    hid_ref[which], down_ref[which, :, columns], preferred_element_type=jnp.float32
                )
            part_ref[j] = total.astype(jnp.bfloat16).reshape(part_ref.shape[1:])
            core_copy(k, j).start()

    for load in loads:
        load.wait()
    compute(last, own_ref)

    @pl.loop(0, tiles)
    def _(j):
        core_copy(last, j).wait()
        acc_ref[j] = part_ref[j, :, core].astype(jnp.float32) + core_ref[last, j].astype(
            jnp.float32
        )

    pool()

    @pl.loop(0, n_ep - 1)
    def _(k):
        gather_copy(k).wait_recv()
        forward_copy(k).start()
        forward_copy(k).wait_recv()
        compute(k, x_ref.at[k])

        @pl.loop(0, tiles)
        def _(j):
            core_copy(k, j).wait()
            core_ref[k, j] = (
                part_ref[j, :, core].astype(jnp.float32) + core_ref[k, j].astype(jnp.float32)
            ).astype(jnp.bfloat16)

        peer_copy(k).start()

    project()

    @pl.loop(0, n_ep - 1)
    def _(k):
        peer_copy(k).wait_recv()
        acc_ref[...] += peer_ref[k].astype(jnp.float32)

    for spot in range(n_z):
        zsend_ref[spot] = acc_ref[:, spot].astype(jnp.bfloat16)
    for k in range(n_z - 1):
        z_copy(k).start()
    total = acc_ref[:, z]
    for k in range(n_z - 1):
        z_copy(k).wait_recv()
        total = total + zrecv_ref[k].astype(jnp.float32)
    squares = jnp.sum(jnp.sum(total * total, axis=0), axis=-1, keepdims=True)
    scale = lax.rsqrt(squares / width + EPS)
    for j in range(tiles):
        columns = slice(j * TILE, (j + 1) * TILE)
        out_ref[:, columns] = (total[j] * scale * gain_ref[:, columns]).astype(jnp.bfloat16)

    @pl.loop(0, n_ep - 1)
    def _(k):
        gather_copy(k).wait_send()
        forward_copy(k).wait_send()
        peer_copy(k).wait_send()

    for k in range(n_z - 1):
        z_copy(k).wait_send()
        weight_copy(k).wait_send()
    for k in range(n_z):
        weight_forward(k).wait_send()
    rim_copy.wait_send()


def fused(operands, n_ep, n_tp):
    expert_in, packed, _, gate_weight, up_weight, down_weight = operands[:6]
    pool_in, out_weight = operands[7], operands[10]
    tokens, wide = expert_in.shape[0], expert_in.shape[1] + packed.shape[1]
    rows, channels = pool_in.shape
    experts, width, units = gate_weight.shape
    tiles, n_z, block = width // TILE, n_tp // 2, tokens // n_tp
    dma = pltpu.SemaphoreType.DMA
    vmem = pl.BlockSpec(memory_space=pltpu.VMEM)
    hbm = pl.BlockSpec(memory_space=pl.ANY)
    bf16 = jnp.bfloat16
    return pl.pallas_call(
        functools.partial(expert_kernel, n_ep, n_tp),
        out_shape=(
            jax.ShapeDtypeStruct((rows, width), bf16),
            jax.ShapeDtypeStruct((block, width), bf16),
        ),
        in_specs=[vmem] * 3 + [hbm] * 3 + [vmem] * 6,
        out_specs=(vmem, vmem),
        scratch_shapes=[
            pltpu.VMEM((tokens, wide), bf16),
            pltpu.VMEM((16, channels), bf16),
            pltpu.VMEM((POOL_ROWS + rows, channels), bf16),
            pltpu.VMEM((rows, channels), bf16),
            pltpu.VMEM((n_tp,) + out_weight.shape, bf16),
            pltpu.VMEM((n_ep - 1, tokens, wide), bf16),
            pltpu.VMEM(gate_weight.shape, bf16),
            pltpu.VMEM(up_weight.shape, bf16),
            pltpu.VMEM(down_weight.shape, bf16),
            pltpu.VMEM((experts, tokens, units), bf16),
            pltpu.VMEM((tiles, n_z, 2, block, TILE), bf16),
            pltpu.VMEM((n_ep, tiles, n_z, block, TILE), bf16),
            pltpu.VMEM((n_ep - 1, tiles, n_z, block, TILE), bf16),
            pltpu.VMEM((tiles, n_z, block, TILE), jnp.float32),
            pltpu.VMEM((n_z, tiles, block, TILE), bf16),
            pltpu.VMEM((n_z - 1, tiles, block, TILE), bf16),
            dma((3,)),
            dma((n_ep - 1,)),
            dma((n_ep - 1,)),
            dma((n_ep - 1,)),
            dma((n_ep - 1,)),
            dma((tiles,)),
            dma((n_ep, tiles)),
            dma((n_ep - 1,)),
            dma((n_ep - 1,)),
            dma((n_z - 1,)),
            dma((n_z - 1,)),
            dma,
            dma,
            dma((n_z - 1,)),
            dma((n_z - 1,)),
            dma((n_z,)),
            dma((n_z,)),
        ],
        compiler_params=pltpu.CompilerParams(
            collective_id=0, has_side_effects=True, vmem_limit_bytes=67043328
        ),
        cost_estimate=pl.CostEstimate(
            flops=6 * n_ep * tokens * experts * units * width,
            bytes_accessed=64 * 2**20,
            transcendentals=0,
        ),
        name="experts",
    )(*operands)


def body(
    pool_in,
    pool_weight,
    pool_gain,
    out_weight,
    mix_gain,
    expert_in,
    routes,
    route_weight,
    pre_gain,
    gate_weight,
    up_weight,
    down_weight,
    post_gain,
):
    n_ep, n_tp = lax.axis_size("ep"), lax.axis_size("tp")
    experts = gate_weight.shape[0] * n_ep
    weights = expert_weights(routes, route_weight, experts)
    high = lax.reduce_precision(weights, 8, 7)
    fill = ((0, 0), (0, LANES // 2 - experts))
    packed = jnp.concatenate([jnp.pad(high, fill), jnp.pad(weights - high, fill)], axis=1)
    operands = (
        expert_in,
        packed.astype(jnp.bfloat16),
        pre_gain[None, :],
        gate_weight,
        up_weight,
        down_weight,
        post_gain[None, :],
        pool_in,
        pool_weight,
        pool_gain[None, :],
        out_weight,
        mix_gain[None, :],
    )
    return fused(operands, n_ep, n_tp)


def solution(mesh):
    return jax.shard_map(
        body,
        mesh=mesh,
        in_specs=(
            P(("ep", "tp"), None),
            P(),
            P(),
            P("tp", None),
            P(),
            P("ep", None),
            P("ep", None),
            P("ep", None),
            P(),
            P("ep", None, "tp"),
            P("ep", None, "tp"),
            P("ep", "tp", None),
            P(),
        ),
        out_specs=(P(("ep", "tp"), None), P(("ep", "tp"), None)),
        check_vma=False,
    )
```
